32 devices in a mesh: grp: 2 (over y), sp: 4 (over z), fs: 2 (over x), tp: 2 (over core).
Axes of the slice: x: 2, y: 2, z: 4, core: 2. Of those that a mesh axis runs over, the one named last changes fastest.
Arguments:
- tokens: bfloat16 [8, 512, 2048], P(('grp', 'fs'), ('sp', 'tp')), parts along dimension 0, may hold values from -24 to 24
- norm_gain: float32 [2048], replicated, may hold values from 0.1 to 1.9
- w_query: bfloat16 [2048, 1024], P(('sp', 'fs'), 'tp'), may hold values from -0.125 to 0.125
- w_key: bfloat16 [2048, 1024], P(('sp', 'fs'), 'tp'), may hold values from -0.125 to 0.125
- w_value: bfloat16 [2048, 1024], P(('sp', 'fs'), 'tp'), may hold values from -0.125 to 0.125
- query_gain: float32 [1024], P('tp'), may hold values from 1 to 26
- key_gain: float32 [1024], P('tp'), may hold values from 0.1 to 1.9
- mix_lambda: float32 [8], P('tp'), may hold values from 0.3 to 0.8
- head_gain: float32 [128], replicated, may hold values from 0.1 to 1.9
- w_gate_b: bfloat16 [2048, 1024], P(('sp', 'fs'), 'tp'), may hold values from -0.125 to 0.125
- w_gate_c: bfloat16 [2048, 1024], P(('sp', 'fs'), 'tp'), may hold values from -0.125 to 0.125
- w_conv_in: bfloat16 [2048, 1024], P(('sp', 'fs'), 'tp'), may hold values from -0.125 to 0.125
- conv_taps: float32 [3, 1024], P(None, 'tp'), may hold values from -3 to 3
- w_out_attn: bfloat16 [1024, 2048], P('tp', ('sp', 'fs')), may hold values from -0.125 to 0.125
- w_out_conv: bfloat16 [1024, 2048], P('tp', ('sp', 'fs')), may hold values from -0.125 to 0.125
Outputs:
- mixed: bfloat16 [8, 512, 2048], P(('grp', 'fs'), ('sp', 'tp')), parts along dimension 0
The draws below stay inside these ranges and needn't reach their ends.
There are 2 independent parts, one for each index of `grp`. The reference program is written for one: setup_inputs(seed, part) draws one part's arguments, and reference() takes and returns one part's arrays. A program takes and returns all parts, laid end to end along the dimension named above; an argument that names none is the same for every part. Nothing has to cross between parts.
All inputs are finite; a program needn't handle non-finite values.
Results may differ from the reference program's by a relative error of at most 0.04.
Values may be sent and summed in bfloat16 or wider, within the bound.
A program may use at most 128 MiB of HBM per device.

```python
import math
import jax
import jax.numpy as jnp
from jax import lax

D = 2048
HEADS = 8
DK = 64
DV = 128
CW = 1024
KW = 3
SEQ_LEN = 512
SEQS = 4


def draw_tokens(key, part):
    first, second, third = jax.random.split(jax.random.fold_in(key, 11), 3)
    shape = (SEQS, SEQ_LEN, D)
    base = jnp.clip(jax.random.normal(first, shape, jnp.float32), -4.0, 4.0)
    row_scale = jnp.exp(jax.random.uniform(second, (SEQS, SEQ_LEN, 1), jnp.float32, math.log(0.3), math.log(3.0)))
    col_scale = jnp.exp(jax.random.uniform(third, (1, 1, D), jnp.float32, math.log(0.5), math.log(2.0)))
    return (base * row_scale * col_scale).astype(jnp.bfloat16)


def draw_query_gain(key, part):
    first = jax.random.fold_in(jax.random.fold_in(key, 23), 0)
    base = 1.7 * jnp.exp(jax.random.uniform(first, (HEADS, 2, DK), jnp.float32, -0.25, 0.25))
    return base.reshape(HEADS * 2 * DK).astype(jnp.float32)


def block_scale(rng, dims, shards, smallest, high):
    loudness, own = 1.0, jax.random.fold_in(rng, 6)
    for dim, shards_of in shards:
        steps = jnp.exp(jax.random.uniform(jax.random.fold_in(own, dim), (shards_of,), jnp.float32, smallest / len(shards), high / len(shards)))
        loudness = loudness * jnp.repeat(steps, dims[dim] // shards_of).reshape([-1 if axis == dim else 1 for axis in range(len(dims))])
    return loudness


def normal_values(key, shape, spread, bound, pieces=(), held_as=jnp.bfloat16):
    array = jax.random.normal(key, shape, jnp.float32) * spread
    if len(pieces) > 0:
        array = block_scale(key, shape, pieces, -0.22, 0.18) * array
    return jnp.clip(array, min=-bound, max=bound).astype(held_as)


def setup_inputs(seed: int = 0, part: int = 0) -> dict:
    keys = jax.random.split(jax.random.key(seed), 16)
    part_splits = jax.random.split(jax.random.fold_in(keys[15], part), 16)
    tokens = draw_tokens(jax.random.fold_in(jax.random.fold_in(keys[15], part), 71), part)
    norm_gain = jnp.clip(1.0 + 0.18 * jax.random.normal(keys[1], (D,), jnp.float32), 0.1, 1.9)
    w_query = normal_values(keys[2], (D, HEADS * 2 * DK), D ** -0.5, 0.125, ((0, 8), (1, 2)))
    w_key = normal_values(keys[3], (D, HEADS * 2 * DK), D ** -0.5, 0.125, ((0, 8), (1, 2)))
    w_value = normal_values(keys[4], (D, HEADS * DV), D ** -0.5, 0.125, ((0, 8), (1, 2)))
    query_gain = draw_query_gain(jax.random.fold_in(keys[15], 71), part)
    key_gain = jnp.clip(1.0 + 0.18 * jax.random.normal(keys[6], (HEADS * 2 * DK,), jnp.float32), 0.1, 1.9)
    mix_lambda = jnp.clip(0.3 + 0.5 * jax.random.uniform(keys[7], (HEADS,), jnp.float32) ** block_scale(keys[7], (HEADS,), ((0, 2),), -0.2, 0.2), 0.3, 0.8)
    head_gain = jnp.clip(1.0 + 0.18 * jax.random.normal(keys[8], (DV,), jnp.float32), 0.1, 1.9)
    w_gate_b = normal_values(keys[9], (D, CW), D ** -0.5, 0.125, ((0, 8), (1, 2)))
    w_gate_c = normal_values(keys[10], (D, CW), D ** -0.5, 0.125, ((0, 8), (1, 2)))
    w_conv_in = normal_values(keys[11], (D, CW), D ** -0.5, 0.125, ((0, 8), (1, 2)))
    conv_taps = normal_values(keys[12], (KW, CW), 0.577, 3.0, ((1, 2),), jnp.float32)
    w_out_attn = normal_values(keys[13], (HEADS * DV, D), (HEADS * DV + CW) ** -0.5, 0.125, ((0, 2), (1, 8)))
    w_out_conv = normal_values(keys[14], (CW, D), (HEADS * DV + CW) ** -0.5, 0.125, ((0, 2), (1, 8)))
    return dict(tokens=tokens, norm_gain=norm_gain, w_query=w_query, w_key=w_key, w_value=w_value, query_gain=query_gain, key_gain=key_gain, mix_lambda=mix_lambda, head_gain=head_gain, w_gate_b=w_gate_b, w_gate_c=w_gate_c, w_conv_in=w_conv_in, conv_taps=conv_taps, w_out_attn=w_out_attn, w_out_conv=w_out_conv)


EPS = 1e-06
NEG = -1e+30
OUT_SCALE = 0.8

def rms_scale(values, gain):
    wide = values.astype(jnp.float32)
    return wide * lax.rsqrt(lax.optimization_barrier(jnp.mean(wide * wide, axis=-1, keepdims=True)) + EPS) * gain.astype(jnp.float32)

def reference(tokens, norm_gain, w_query, w_key, w_value, query_gain, key_gain, mix_lambda, head_gain, w_gate_b, w_gate_c, w_conv_in, conv_taps, w_out_attn, w_out_conv):
    length = SEQ_LEN
    block = math.gcd(length, 512)

    def one(seq):
        normed = rms_scale(seq, norm_gain).astype(jnp.bfloat16)

        def project(weight):
            return jnp.dot(normed, weight, preferred_element_type=jnp.float32).astype(jnp.bfloat16)
        query = rms_scale(project(w_query).reshape(length, HEADS, 2, DK), query_gain.reshape(HEADS, 2, DK)).astype(jnp.bfloat16)
        key = rms_scale(project(w_key).reshape(length, HEADS, 2, DK), key_gain.reshape(HEADS, 2, DK)).astype(jnp.bfloat16)
        value = project(w_value).reshape(length, HEADS, DV)
        key_wide = key.astype(jnp.float32)
        value_wide = value.astype(jnp.float32)
        key_pos = jnp.arange(length, dtype=jnp.int32)

        def attend(start):
            q_block = lax.dynamic_slice_in_dim(query, start, block, 0).astype(jnp.float32)
            q_pos = start + jnp.arange(block, dtype=jnp.int32)
            score = jnp.einsum('qhmd,khmd->hmqk', q_block, key_wide) * DK ** (-0.5)
            allowed = key_pos[None, :] <= q_pos[:, None]
            score = jnp.where(allowed, score, NEG)
            top = lax.optimization_barrier(jnp.max(score, axis=-1, keepdims=True))
            weights = jnp.exp(score - top)
            total = lax.optimization_barrier(jnp.sum(weights, axis=-1))
            rounded = lax.optimization_barrier(weights.astype(jnp.bfloat16)).astype(jnp.float32)
            summed = jnp.einsum('hmqk,khd->hmqd', rounded, value_wide)
            head_map = summed / total[..., None]
            differ = head_map[:, 0] - mix_lambda.astype(jnp.float32)[:, None, None] * head_map[:, 1]
            normal = rms_scale(differ, head_gain) * OUT_SCALE
            return normal.transpose(1, 0, 2).reshape(block, HEADS * DV).astype(jnp.bfloat16)
        starts = jnp.arange(length // block, dtype=jnp.int32) * block
        attn = lax.map(attend, starts).reshape(length, HEADS * DV)
        gate_b = project(w_gate_b)
        gate_c = project(w_gate_c)
        conv_in = project(w_conv_in)
        shaped = (gate_c.astype(jnp.float32) * conv_in.astype(jnp.float32)).astype(jnp.bfloat16)
        padded = jnp.concatenate([jnp.zeros((KW - 1, CW), jnp.bfloat16), shaped], axis=0).astype(jnp.float32)
        conv = jnp.zeros((length, CW), jnp.float32)
        for tap in range(KW):
            conv = conv + conv_taps[tap].astype(jnp.float32) * padded[tap:tap + length]
        conv_out = (gate_b.astype(jnp.float32) * conv).astype(jnp.bfloat16)
        total_out = jnp.dot(attn, w_out_attn, preferred_element_type=jnp.float32) + jnp.dot(conv_out, w_out_conv, preferred_element_type=jnp.float32)
        return total_out.astype(jnp.bfloat16)
    return lax.map(one, tokens)
```

```python
import functools
import math

import jax
import jax.numpy as jnp
from jax import lax
from jax.experimental import pallas as pl
from jax.experimental.pallas import tpu as pltpu
from jax.sharding import PartitionSpec as P

DK = 64
DV = 128
KW = 3


EPS = 1e-06
NEG = -1e30
OUT_SCALE = 0.8


def from_behind(block, axis, distance):
    devices = range(lax.axis_size(axis))
    route = [(i - distance, i) for i in devices if i - distance in devices]
    return lax.ppermute(block, axis, route)


def rms_scale(values, gain):
    wide = values.astype(jnp.float32)
    return wide * lax.rsqrt(jnp.mean(wide * wide, axis=-1, keepdims=True) + EPS) * gain


def attend_heads(normed, wq_full, wk_full, wv_full, query_gain, key_gain, mix_lambda, head_gain):
    rows = normed.shape[0]
    heads_here = mix_lambda.shape[0]
    query = rms_scale(
        jnp.dot(normed, wq_full, preferred_element_type=jnp.float32)
        .astype(jnp.bfloat16)
        .reshape(rows, heads_here, 2, DK),
        query_gain.reshape(heads_here, 2, DK),
    ).astype(jnp.bfloat16)
    key = rms_scale(
        jnp.dot(normed, wk_full, preferred_element_type=jnp.float32)
        .astype(jnp.bfloat16)
        .reshape(rows, heads_here, 2, DK),
        key_gain.reshape(heads_here, 2, DK),
    ).astype(jnp.bfloat16)
    value = jnp.dot(normed, wv_full, preferred_element_type=jnp.float32).astype(jnp.bfloat16)
    q_pos = lax.axis_index("sp") * rows + jnp.arange(rows, dtype=jnp.int32)
    init = (
        jnp.full((heads_here, 2, rows), NEG, jnp.float32),
        jnp.zeros((heads_here, 2, rows), jnp.float32),
        jnp.zeros((heads_here, 2, rows, DV), jnp.float32),
    )
    key_piece = lax.all_gather(key.reshape(rows, heads_here * 2 * DK), "sp", axis=0, tiled=True)
    value_piece = lax.all_gather(value, "sp", axis=0, tiled=True)
    count = key_piece.shape[0]
    width = math.gcd(count, 1024)
    blocks = count // width
    key_blocks = key_piece.reshape(blocks, width, heads_here, 2, DK)
    value_blocks = value_piece.reshape(blocks, width, heads_here, DV)
    begins = jnp.arange(blocks, dtype=jnp.int32) * width

    def step(state, inputs):
        running, total, summed = state
        key_block, value_block, begin = inputs
        k_pos = begin + jnp.arange(width, dtype=jnp.int32)
        score = jnp.einsum(
            "qhmd,khmd->hmqk", query, key_block, preferred_element_type=jnp.float32
        ) * DK ** (-0.5)
        allowed = k_pos[None, :] <= q_pos[:, None]
        score = jnp.where(allowed, score, NEG)
        newest = jnp.maximum(running, jnp.max(score, axis=-1))
        factor = jnp.exp(running - newest)
        weights = jnp.where(allowed, jnp.exp(score - newest[..., None]), 0.0)
        total = total * factor + jnp.sum(weights, axis=-1)
        summed = summed * factor[..., None] + jnp.einsum(
            "hmqk,khd->hmqd",
            weights.astype(jnp.bfloat16),
            value_block,
            preferred_element_type=jnp.float32,
        )
        return ((newest, total, summed), None)

    result, unused = lax.scan(step, init, (key_blocks, value_blocks, begins))
    running, total, summed = result
    head_map = summed / total[..., None]
    differ = head_map[:, 0] - mix_lambda[:, None, None] * head_map[:, 1]
    normal = rms_scale(differ, head_gain) * OUT_SCALE
    return normal.transpose(1, 0, 2).reshape(rows, heads_here * DV).astype(jnp.bfloat16)


def gated_conv(normed, wb_full, wc_full, wi_full, conv_taps):
    rows = normed.shape[0]
    gate_b = jnp.dot(normed, wb_full, preferred_element_type=jnp.float32).astype(jnp.bfloat16)
    gate_c = jnp.dot(normed, wc_full, preferred_element_type=jnp.float32).astype(jnp.bfloat16)
    conv_in = jnp.dot(normed, wi_full, preferred_element_type=jnp.float32).astype(jnp.bfloat16)
    shaped = (gate_c.astype(jnp.float32) * conv_in.astype(jnp.float32)).astype(jnp.bfloat16)
    edge = from_behind(shaped[rows - (KW - 1) :], "sp", 1)
    padded = jnp.concatenate([edge, shaped], axis=0).astype(jnp.float32)
    conv = conv_taps[0][None, :] * padded[0:rows]
    for tap in range(1, KW):
        conv = conv + conv_taps[tap][None, :] * padded[tap : tap + rows]
    return (gate_b.astype(jnp.float32) * conv).astype(jnp.bfloat16)


def normalize_rows(own_rows, norm_gain):
    return rms_scale(lax.all_gather(own_rows, "tp", axis=0, tiled=True), norm_gain).astype(
        jnp.bfloat16
    )


def gather_on_device(
    tokens,
    norm_gain,
    w_query,
    w_key,
    w_value,
    query_gain,
    key_gain,
    mix_lambda,
    head_gain,
    w_gate_b,
    w_gate_c,
    w_conv_in,
    conv_taps,
    w_out_attn,
    w_out_conv,
):
    seq_count = tokens.shape[0]
    gathered = (
        lax.all_gather(w_query, ("sp", "fs"), axis=0, tiled=True),
        lax.all_gather(w_key, ("sp", "fs"), axis=0, tiled=True),
        lax.all_gather(w_value, ("sp", "fs"), axis=0, tiled=True),
        lax.all_gather(w_gate_b, ("sp", "fs"), axis=0, tiled=True),
        lax.all_gather(w_gate_c, ("sp", "fs"), axis=0, tiled=True),
        lax.all_gather(w_conv_in, ("sp", "fs"), axis=0, tiled=True),
        lax.all_gather(w_out_attn, ("sp", "fs"), axis=1, tiled=True),
        lax.all_gather(w_out_conv, ("sp", "fs"), axis=1, tiled=True),
    )
    normed_list = [normalize_rows(tokens[index], norm_gain) for index in range(seq_count)]
    attn_list = [
        attend_heads(
            normed,
            gathered[0],
            gathered[1],
            gathered[2],
            query_gain,
            key_gain,
            mix_lambda,
            head_gain,
        )
        for normed in normed_list
    ]
    conv_list = [
        gated_conv(normed, gathered[3], gathered[4], gathered[5], conv_taps)
        for normed in normed_list
    ]
    out_attn = gathered[6]
    out_conv = gathered[7]
    results = []
    for index in range(seq_count):
        attn = attn_list[index]
        conv_out = conv_list[index]
        results.append(
            lax.psum_scatter(
                (
                    jnp.dot(attn, out_attn, preferred_element_type=jnp.float32)
                    + jnp.dot(conv_out, out_conv, preferred_element_type=jnp.float32)
                ).astype(jnp.bfloat16),
                "tp",
                scatter_dimension=0,
                tiled=True,
            )
        )
    return jnp.stack(results, axis=0)


MESH = pl.DeviceIdType.MESH


def greet(peers):
    barrier = pltpu.get_barrier_semaphore()
    for peer in peers:
        pl.semaphore_signal(barrier, inc=1, device_id=peer, device_id_type=MESH)
    pl.semaphore_wait(barrier, len(peers))


def remote(src, dst, send, recv, peer):
    return pltpu.make_async_remote_copy(
        src_ref=src, dst_ref=dst, send_sem=send, recv_sem=recv, device_id=peer, device_id_type=MESH
    )


def gather_kernel(
    tok_ref, w_ref, o_ref, tok_all, w_all, o_all,
    send_z, recv_z, send_t, recv_t, send_x, recv_x, send_y, recv_y, local,
):
    sp, fs = lax.axis_size("sp"), lax.axis_size("fs")
    s, f = lax.axis_index("sp"), lax.axis_index("fs")
    g, t = lax.axis_index("grp"), lax.axis_index("tp")
    width = o_ref.shape[1]
    z_peers = [{"sp": lax.rem(s + d, sp)} for d in range(1, sp)]
    x_peers = [{"fs": lax.rem(f + d, fs)} for d in range(1, fs)]
    y_peer = {"grp": 1 - g}
    t_peer = {"tp": 1 - t}
    greet(z_peers + x_peers + [y_peer, t_peer])

    def tok_at(sv, tv):
        return tok_all.at[:, sv * 2 + tv]

    def w_at(gv, sv, fv):
        return w_all.at[gv, sv * fs + fv]

    def o_at(gv, sv, fv):
        begin = pl.multiple_of((sv * fs + fv) * width, 128)
        return o_all.at[gv, :, pl.ds(begin, width)]

    started = []

    def go(copy):
        copy.start()
        started.append(copy)

    for d in range(1, sp):
        to = lax.rem(s + d, sp)
        peer = {"sp": to}
        go(remote(tok_ref, tok_at(s, t), send_z.at[0, d], recv_z.at[0, d], peer))
        go(remote(w_ref.at[to], w_at(g, s, f), send_z.at[1, d], recv_z.at[1, d], peer))
        go(remote(o_ref, o_at(g, s, f), send_z.at[2, d], recv_z.at[2, d], peer))
    keep = [
        pltpu.make_async_copy(tok_ref, tok_at(s, t), local.at[0]),
        pltpu.make_async_copy(w_ref.at[s], w_at(g, s, f), local.at[1]),
        pltpu.make_async_copy(o_ref, o_at(g, s, f), local.at[2]),
    ]
    for copy in keep:
        copy.start()

    def z_wait(kind, d, ref):
        remote(ref, ref, send_z.at[kind, d], recv_z.at[kind, d], t_peer).wait_recv()

    for d in range(sp):
        sv = lax.rem(s + sp - d, sp)
        if d:
            z_wait(0, d, tok_at(sv, t))
        src = tok_at(sv, t) if d else tok_ref
        go(remote(src, tok_at(sv, t), send_t.at[d], recv_t.at[d], t_peer))
        if d:
            z_wait(1, d, w_at(g, sv, f))
        src = w_at(g, sv, f) if d else w_ref.at[s]
        go(remote(src, w_at(g, sv, f), send_y.at[0, d], recv_y.at[0, d], y_peer))
        for e, peer in enumerate(x_peers):
            go(remote(src, w_at(g, sv, f), send_x.at[0, 0, d, e], recv_x.at[0, 0, d, e], peer))
        if d:
            z_wait(2, d, o_at(g, sv, f))
        src = o_at(g, sv, f) if d else o_ref
        go(remote(src, o_at(g, sv, f), send_y.at[1, d], recv_y.at[1, d], y_peer))
        for e, peer in enumerate(x_peers):
            go(remote(src, o_at(g, sv, f), send_x.at[1, 0, d, e], recv_x.at[1, 0, d, e], peer))
    for d in range(sp):
        sv = lax.rem(s + sp - d, sp)
        for kind, at in enumerate((w_at, o_at)):
            ref = at(1 - g, sv, f)
            remote(ref, ref, send_y.at[kind, d], recv_y.at[kind, d], y_peer).wait_recv()
            for e, peer in enumerate(x_peers):
                go(remote(ref, ref, send_x.at[kind, 1, d, e], recv_x.at[kind, 1, d, e], peer))
    for d in range(sp):
        sv = lax.rem(s + sp - d, sp)
        ref = tok_at(sv, 1 - t)
        remote(ref, ref, send_t.at[d], recv_t.at[d], t_peer).wait_recv()
        for kind, at in enumerate((w_at, o_at)):
            for turn, gv in enumerate((g, 1 - g)):
                for e in range(fs - 1):
                    fv = lax.rem(f + fs - 1 - e, fs)
                    ref = at(gv, sv, fv)
                    remote(
                        ref, ref, send_x.at[kind, turn, d, e], recv_x.at[kind, turn, d, e], t_peer
                    ).wait_recv()
    for copy in started:
        copy.wait_send()
    for copy in keep:
        copy.wait()


def gather_all(normed, w_half, o_half, sp, fs):
    seqs, rows, wide = normed.shape
    any_spec = pl.BlockSpec(memory_space=pl.ANY)
    dma = pltpu.SemaphoreType.DMA
    return pl.pallas_call(
        gather_kernel,
        out_shape=(
            jax.ShapeDtypeStruct((seqs, sp * 2, rows, wide), jnp.bfloat16),
            jax.ShapeDtypeStruct((2, sp * fs) + w_half.shape[1:], jnp.bfloat16),
            jax.ShapeDtypeStruct((2, o_half.shape[0], o_half.shape[1] * sp * fs), jnp.bfloat16),
        ),
        in_specs=[any_spec] * 3,
        out_specs=[any_spec] * 3,
        scratch_shapes=[
            dma((3, sp)), dma((3, sp)), dma((sp,)), dma((sp,)),
            dma((2, 2, sp, fs - 1)), dma((2, 2, sp, fs - 1)),
            dma((2, sp)), dma((2, sp)), dma((3,)),
        ],
        compiler_params=pltpu.CompilerParams(collective_id=0, has_side_effects=True),
        name="gather_all",
    )(normed, w_half, o_half)


def merge_kernel(
    attn_ref, conv_ref, o_ref, out_ref, feats, weights, mine, theirs, got, send, recv, swap, local,
):
    sp = lax.axis_size("sp")
    s, t = lax.axis_index("sp"), lax.axis_index("tp")
    z_peers = [{"sp": lax.rem(s + d, sp)} for d in range(1, sp)]
    t_peer = {"tp": 1 - t}
    greet(z_peers + [t_peer])
    seqs, unused, rows, wide = attn_ref.shape
    fetch = pltpu.make_async_copy(o_ref, weights, local.at[2])
    started = []
    for d in range(1, sp):
        to = lax.rem(s + d, sp)
        for kind, ref in enumerate((attn_ref, conv_ref)):
            copy = remote(
                ref.at[:, to], feats.at[kind, s], send.at[kind, d], recv.at[kind, d], {"sp": to}
            )
            copy.start()
            started.append(copy)
    fetch.start()
    keep = [
        pltpu.make_async_copy(ref.at[:, s], feats.at[kind, s], local.at[kind])
        for kind, ref in enumerate((attn_ref, conv_ref))
    ]
    for copy in keep:
        copy.start()
    for copy in keep:
        copy.wait()
    for copy in started:
        copy.wait()
    fetch.wait()
    half = rows // 2
    piece = 512 if weights.shape[2] % 512 == 0 else weights.shape[2]

    def product(tv, begin):
        total = jnp.zeros((seqs * half, piece), jnp.float32)
        for kind in range(2):
            left = jnp.concatenate(
                [
                    feats[kind, sv, :, pl.ds(pl.multiple_of(tv * half, half), half), :].reshape(
                        seqs * half, wide
                    )
                    for sv in range(sp)
                ],
                axis=1,
            )
            total = total + jnp.dot(
                left, weights[kind, :, pl.ds(begin, piece)], preferred_element_type=jnp.float32
            )
        return total

    copies = []
    for turn in range(weights.shape[2] // piece):
        theirs[turn] = product(1 - t, turn * piece).astype(jnp.bfloat16)
        copy = remote(theirs.at[turn], got.at[turn], swap.at[0, turn], swap.at[1, turn], t_peer)
        copy.start()
        copies.append(copy)
    for turn in range(weights.shape[2] // piece):
        mine[turn] = product(t, turn * piece)
    for turn, copy in enumerate(copies):
        copy.wait()
        total = mine[turn] + got[turn].astype(jnp.float32)
        out_ref[:, :, pl.ds(turn * piece, piece)] = total.astype(jnp.bfloat16).reshape(
            seqs, half, piece
        )


def merge(attn, conv_out, o_all):
    seqs, sp, rows, wide = attn.shape
    columns = o_all.shape[2]
    piece = 512 if columns % 512 == 0 else columns
    turns = columns // piece
    half = rows // 2
    any_spec = pl.BlockSpec(memory_space=pl.ANY)
    dma = pltpu.SemaphoreType.DMA
    return pl.pallas_call(
        merge_kernel,
        out_shape=jax.ShapeDtypeStruct((seqs, half, columns), jnp.bfloat16),
        in_specs=[any_spec] * 3,
        out_specs=pl.BlockSpec(memory_space=pltpu.VMEM),
        scratch_shapes=[
            pltpu.VMEM((2, sp, seqs, rows, wide), jnp.bfloat16),
            pltpu.VMEM(o_all.shape, jnp.bfloat16),
            pltpu.VMEM((turns, seqs * half, piece), jnp.float32),
            pltpu.VMEM((turns, seqs * half, piece), jnp.bfloat16),
            pltpu.VMEM((turns, seqs * half, piece), jnp.bfloat16),
            dma((2, sp)), dma((2, sp)), dma((2, turns)), dma((3,)),
        ],
        compiler_params=pltpu.CompilerParams(collective_id=1, has_side_effects=True),
        name="merge",
    )(attn, conv_out, o_all)


def head_map(query, key, value, mix, head_gain):
    seqs, count = value.shape[0], value.shape[1]
    score = jnp.einsum("bqmd,bkmd->bmqk", query, key, preferred_element_type=jnp.float32)
    score = score * DK ** (-0.5)
    place = jnp.arange(count, dtype=jnp.int32)
    score = jnp.where(place[None, :] <= place[:, None], score, NEG)
    weights = jnp.exp(score - jnp.max(score, axis=-1, keepdims=True))
    total = jnp.sum(weights, axis=-1)
    summed = jnp.einsum(
        "bmqk,bkd->bmqd", weights.astype(jnp.bfloat16), value, preferred_element_type=jnp.float32
    )
    mapped = summed / total[..., None]
    return (rms_scale(mapped[:, 0] - mix * mapped[:, 1], head_gain) * OUT_SCALE).astype(jnp.bfloat16)


def heads_on_device(
    tokens, norm_gain, w_query, w_key, w_value, query_gain, key_gain, mix_lambda, head_gain,
    w_gate_b, w_gate_c, w_conv_in, conv_taps, w_out_attn, w_out_conv,
):
    sp, fs = lax.axis_size("sp"), lax.axis_size("fs")
    s, first = lax.axis_index("sp"), lax.axis_index("grp") == 0
    seqs, rows, wide = tokens.shape
    normed = rms_scale(tokens, norm_gain).astype(jnp.bfloat16)
    depth, columns = w_query.shape
    each = columns // sp

    def half(pair):
        return jnp.where(first, pair[0], pair[1])

    picked = [
        half(pair).reshape(depth, sp, each)
        for pair in ((w_query, w_gate_b), (w_key, w_gate_c), (w_value, w_conv_in))
    ]
    w_half = jnp.stack(picked, axis=2).transpose(1, 0, 2, 3).reshape(sp, depth, 3 * each)
    o_half = half((w_out_attn, w_out_conv))
    tok_all, w_all, o_all = gather_all(normed, w_half, o_half, sp, fs)
    count = rows * sp * 2
    x = tok_all.reshape(seqs * count, wide)

    def project(index):
        out = jnp.dot(
            x, w_all[index].reshape(wide, 3 * each), preferred_element_type=jnp.float32
        ).astype(jnp.bfloat16)
        return [out[:, n * each : (n + 1) * each].reshape(seqs, count, each) for n in range(3)]

    query_raw, key_raw, value = project(0)
    gate_b, gate_c, conv_in = project(1)

    def mine(array, axis=0):
        return lax.dynamic_slice_in_dim(array, s * each, each, axis)

    query = rms_scale(
        query_raw.reshape(seqs, count, 2, DK), mine(query_gain).reshape(2, DK)
    ).astype(jnp.bfloat16)
    key = rms_scale(
        key_raw.reshape(seqs, count, 2, DK), mine(key_gain).reshape(2, DK)
    ).astype(jnp.bfloat16)
    mix = lax.dynamic_slice_in_dim(mix_lambda, s, 1)[0]
    attn = head_map(query, key, value, mix, head_gain)
    shaped = (gate_c.astype(jnp.float32) * conv_in.astype(jnp.float32)).astype(jnp.bfloat16)
    padded = jnp.pad(shaped, ((0, 0), (KW - 1, 0), (0, 0))).astype(jnp.float32)
    taps = mine(conv_taps, 1)
    conv = taps[0] * padded[:, 0:count]
    for tap in range(1, KW):
        conv = conv + taps[tap] * padded[:, tap : tap + count]
    conv_out = (gate_b.astype(jnp.float32) * conv).astype(jnp.bfloat16)
    shape = (seqs, sp, rows * 2, each)
    return merge(attn.reshape(shape), conv_out.reshape(shape), o_all)


def on_device(*arrays):
    heads_here, channels = arrays[7].shape[0], arrays[12].shape[1]
    sizes = [lax.axis_size(axis) for axis in ("grp", "tp", "fs", "sp")]
    whole_heads = heads_here == sizes[3] and channels == heads_here * DV
    if whole_heads and sizes[0] == 2 and sizes[1] == 2 and sizes[2] > 1:
        return heads_on_device(*arrays)
    return gather_on_device(*arrays)


def solution(mesh):
    placed = (
        P(("grp", "fs"), ("sp", "tp"), None),
        P(),
        P(("sp", "fs"), "tp"),
        P(("sp", "fs"), "tp"),
        P(("sp", "fs"), "tp"),
        P("tp"),
        P("tp"),
        P("tp"),
        P(),
        P(("sp", "fs"), "tp"),
        P(("sp", "fs"), "tp"),
        P(("sp", "fs"), "tp"),
        P(None, "tp"),
        P("tp", ("sp", "fs")),
        P("tp", ("sp", "fs")),
    )
    return jax.shard_map(
        on_device,
        mesh=mesh,
        in_specs=placed,
        out_specs=P(("grp", "fs"), ("sp", "tp"), None),
        check_vma=False,
    )
```

```python
import functools
import math

import jax
import jax.numpy as jnp
from jax import lax
from jax.experimental import pallas as pl
from jax.experimental.pallas import tpu as pltpu
from jax.sharding import PartitionSpec as P

DK = 64
DV = 128
KW = 3


EPS = 1e-06
NEG = -1e30
OUT_SCALE = 0.8


def from_behind(block, axis, distance):
    devices = range(lax.axis_size(axis))
    route = [(i - distance, i) for i in devices if i - distance in devices]
    return lax.ppermute(block, axis, route)


def rms_scale(values, gain):
    wide = values.astype(jnp.float32)
    return wide * lax.rsqrt(jnp.mean(wide * wide, axis=-1, keepdims=True) + EPS) * gain


def attend_heads(normed, wq_full, wk_full, wv_full, query_gain, key_gain, mix_lambda, head_gain):
    rows = normed.shape[0]
    heads_here = mix_lambda.shape[0]
    query = rms_scale(
        jnp.dot(normed, wq_full, preferred_element_type=jnp.float32)
        .astype(jnp.bfloat16)
        .reshape(rows, heads_here, 2, DK),
        query_gain.reshape(heads_here, 2, DK),
    ).astype(jnp.bfloat16)
    key = rms_scale(
        jnp.dot(normed, wk_full, preferred_element_type=jnp.float32)
        .astype(jnp.bfloat16)
        .reshape(rows, heads_here, 2, DK),
        key_gain.reshape(heads_here, 2, DK),
    ).astype(jnp.bfloat16)
    value = jnp.dot(normed, wv_full, preferred_element_type=jnp.float32).astype(jnp.bfloat16)
    q_pos = lax.axis_index("sp") * rows + jnp.arange(rows, dtype=jnp.int32)
    init = (
        jnp.full((heads_here, 2, rows), NEG, jnp.float32),
        jnp.zeros((heads_here, 2, rows), jnp.float32),
        jnp.zeros((heads_here, 2, rows, DV), jnp.float32),
    )
    key_piece = lax.all_gather(key.reshape(rows, heads_here * 2 * DK), "sp", axis=0, tiled=True)
    value_piece = lax.all_gather(value, "sp", axis=0, tiled=True)
    count = key_piece.shape[0]
    width = math.gcd(count, 1024)
    blocks = count // width
    key_blocks = key_piece.reshape(blocks, width, heads_here, 2, DK)
    value_blocks = value_piece.reshape(blocks, width, heads_here, DV)
    begins = jnp.arange(blocks, dtype=jnp.int32) * width

    def step(state, inputs):
        running, total, summed = state
        key_block, value_block, begin = inputs
        k_pos = begin + jnp.arange(width, dtype=jnp.int32)
        score = jnp.einsum(
            "qhmd,khmd->hmqk", query, key_block, preferred_element_type=jnp.float32
        ) * DK ** (-0.5)
        allowed = k_pos[None, :] <= q_pos[:, None]
        score = jnp.where(allowed, score, NEG)
        newest = jnp.maximum(running, jnp.max(score, axis=-1))
        factor = jnp.exp(running - newest)
        weights = jnp.where(allowed, jnp.exp(score - newest[..., None]), 0.0)
        total = total * factor + jnp.sum(weights, axis=-1)
        summed = summed * factor[..., None] + jnp.einsum(
            "hmqk,khd->hmqd",
            weights.astype(jnp.bfloat16),
            value_block,
            preferred_element_type=jnp.float32,
        )
        return ((newest, total, summed), None)

    result, unused = lax.scan(step, init, (key_blocks, value_blocks, begins))
    running, total, summed = result
    head_map = summed / total[..., None]
    differ = head_map[:, 0] - mix_lambda[:, None, None] * head_map[:, 1]
    normal = rms_scale(differ, head_gain) * OUT_SCALE
    return normal.transpose(1, 0, 2).reshape(rows, heads_here * DV).astype(jnp.bfloat16)


def gated_conv(normed, wb_full, wc_full, wi_full, conv_taps):
    rows = normed.shape[0]
    gate_b = jnp.dot(normed, wb_full, preferred_element_type=jnp.float32).astype(jnp.bfloat16)
    gate_c = jnp.dot(normed, wc_full, preferred_element_type=jnp.float32).astype(jnp.bfloat16)
    conv_in = jnp.dot(normed, wi_full, preferred_element_type=jnp.float32).astype(jnp.bfloat16)
    shaped = (gate_c.astype(jnp.float32) * conv_in.astype(jnp.float32)).astype(jnp.bfloat16)
    edge = from_behind(shaped[rows - (KW - 1) :], "sp", 1)
    padded = jnp.concatenate([edge, shaped], axis=0).astype(jnp.float32)
    conv = conv_taps[0][None, :] * padded[0:rows]
    for tap in range(1, KW):
        conv = conv + conv_taps[tap][None, :] * padded[tap : tap + rows]
    return (gate_b.astype(jnp.float32) * conv).astype(jnp.bfloat16)


def normalize_rows(own_rows, norm_gain):
    return rms_scale(lax.all_gather(own_rows, "tp", axis=0, tiled=True), norm_gain).astype(
        jnp.bfloat16
    )


def gather_on_device(
    tokens,
    norm_gain,
    w_query,
    w_key,
    w_value,
    query_gain,
    key_gain,
    mix_lambda,
    head_gain,
    w_gate_b,
    w_gate_c,
    w_conv_in,
    conv_taps,
    w_out_attn,
    w_out_conv,
):
    seq_count = tokens.shape[0]
    gathered = (
        lax.all_gather(w_query, ("sp", "fs"), axis=0, tiled=True),
        lax.all_gather(w_key, ("sp", "fs"), axis=0, tiled=True),
        lax.all_gather(w_value, ("sp", "fs"), axis=0, tiled=True),
        lax.all_gather(w_gate_b, ("sp", "fs"), axis=0, tiled=True),
        lax.all_gather(w_gate_c, ("sp", "fs"), axis=0, tiled=True),
        lax.all_gather(w_conv_in, ("sp", "fs"), axis=0, tiled=True),
        lax.all_gather(w_out_attn, ("sp", "fs"), axis=1, tiled=True),
        lax.all_gather(w_out_conv, ("sp", "fs"), axis=1, tiled=True),
    )
    normed_list = [normalize_rows(tokens[index], norm_gain) for index in range(seq_count)]
    attn_list = [
        attend_heads(
            normed,
            gathered[0],
            gathered[1],
            gathered[2],
            query_gain,
            key_gain,
            mix_lambda,
            head_gain,
        )
        for normed in normed_list
    ]
    conv_list = [
        gated_conv(normed, gathered[3], gathered[4], gathered[5], conv_taps)
        for normed in normed_list
    ]
    out_attn = gathered[6]
    out_conv = gathered[7]
    results = []
    for index in range(seq_count):
        attn = attn_list[index]
        conv_out = conv_list[index]
        results.append(
            lax.psum_scatter(
                (
                    jnp.dot(attn, out_attn, preferred_element_type=jnp.float32)
                    + jnp.dot(conv_out, out_conv, preferred_element_type=jnp.float32)
                ).astype(jnp.bfloat16),
                "tp",
                scatter_dimension=0,
                tiled=True,
            )
        )
    return jnp.stack(results, axis=0)


MESH = pl.DeviceIdType.MESH


def greet(peers):
    barrier = pltpu.get_barrier_semaphore()
    for peer in peers:
        pl.semaphore_signal(barrier, inc=1, device_id=peer, device_id_type=MESH)
    pl.semaphore_wait(barrier, len(peers))


def remote(src, dst, send, recv, peer):
    return pltpu.make_async_remote_copy(
        src_ref=src, dst_ref=dst, send_sem=send, recv_sem=recv, device_id=peer, device_id_type=MESH
    )


def gather_kernel(
    tok_ref, w_ref, o_ref, tok_all, w_all, o_all,
    send_z, recv_z, send_c, recv_c, send_t, recv_t, send_x, recv_x, send_y, recv_y, local,
):
    sp, fs = lax.axis_size("sp"), lax.axis_size("fs")
    s, f = lax.axis_index("sp"), lax.axis_index("fs")
    g, t = lax.axis_index("grp"), lax.axis_index("tp")
    width = o_ref.shape[1]
    z_peers = [{"sp": lax.rem(s + d, sp)} for d in range(1, sp)]
    x_peers = [{"fs": lax.rem(f + d, fs)} for d in range(1, fs)]
    y_peer = {"grp": 1 - g}
    t_peer = {"tp": 1 - t}
    greet(z_peers + x_peers + [y_peer, t_peer])

    def tok_at(sv, tv):
        return tok_all.at[:, sv * 2 + tv]

    def w_at(gv, sv, fv):
        return w_all.at[gv, sv * fs + fv]

    def o_at(gv, sv):
        return o_all.at[gv, :, pl.ds(pl.multiple_of(sv * width, 128), width)]

    started = []

    def go(copy, needs=()):
        def run(act):
            if needs:
                pl.when(functools.reduce(jnp.logical_and, needs))(act)
            else:
                act()

        run(copy.start)
        started.append((run, copy))

    def arrived(sem, ref, needs=()):
        copy = remote(ref, ref, sem, sem, t_peer)
        if needs:
            pl.when(functools.reduce(jnp.logical_and, needs))(copy.wait_recv)
        else:
            copy.wait_recv()

    def chain(kind, at, src, sv, needs):
        ref = at(sv)
        for way, (to, moves) in enumerate(((s + 1, sv <= s), (s - 1, sv >= s))):
            fits = to < sp if way == 0 else to >= 0
            peer = {"sp": jnp.clip(to, 0, sp - 1)}
            go(
                remote(src, ref, send_c.at[kind, way, sv], recv_c.at[kind, sv], peer),
                needs + [fits, moves],
            )

    def spread_w(d, src):
        sv = lax.rem(s + sp - d, sp)
        for e, peer in enumerate(x_peers):
            go(remote(src, w_at(g, sv, f), send_x.at[0, d, e], recv_x.at[0, d, e], peer))
        go(remote(src, w_at(g, sv, f), send_y.at[0, d], recv_y.at[0, d], y_peer))

    def tok_mine(sv):
        return tok_at(sv, t)

    def o_mine(sv):
        return o_at(g, sv)

    for d in range(1, sp):
        to = lax.rem(s + d, sp)
        go(remote(w_ref.at[to], w_at(g, s, f), send_z.at[d], recv_z.at[d], {"sp": to}))
    chain(0, tok_mine, tok_ref, s, [])
    spread_w(0, w_ref.at[s])
    go(remote(tok_ref, tok_mine(s), send_t.at[s], recv_t.at[s], t_peer))
    keep = [
        pltpu.make_async_copy(tok_ref, tok_at(s, t), local.at[0]),
        pltpu.make_async_copy(w_ref.at[s], w_at(g, s, f), local.at[1]),
        pltpu.make_async_copy(o_ref, o_at(g, s), local.at[2]),
    ]
    for copy in keep:
        copy.start()
    for d in range(1, sp):
        ref = w_at(g, lax.rem(s + sp - d, sp), f)
        arrived(recv_z.at[d], ref)
        spread_w(d, ref)

    def around(kind, at, distance, beyond):
        for shift in (-distance, distance):
            sv = jnp.clip(s + shift, 0, sp - 1)
            there = (s + shift >= 0) if shift < 0 else (s + shift < sp)
            ref = at(sv)
            arrived(recv_c.at[kind, sv], ref, [there])
            if shift < 0:
                to, fits, way = s + 1, s + 1 < sp, 0
            else:
                to, fits, way = s - 1, s - 1 >= 0, 1
            peer = {"sp": jnp.clip(to, 0, sp - 1)}
            go(
                remote(ref, ref, send_c.at[kind, way, sv], recv_c.at[kind, sv], peer),
                [there, fits],
            )
            beyond(sv, ref, there)

    def tok_beyond(sv, ref, there):
        go(remote(ref, ref, send_t.at[sv], recv_t.at[sv], t_peer), [there])

    def o_beyond(sv, ref, there):
        go(remote(ref, ref, send_y.at[1, sv], recv_y.at[1, sv], y_peer), [there])

    for k in range(1, sp):
        around(0, tok_mine, k, tok_beyond)
        if k == 1:
            for d in range(sp):
                ref = w_at(1 - g, lax.rem(s + sp - d, sp), f)
                arrived(recv_y.at[0, d], ref)
                for e, peer in enumerate(x_peers):
                    go(remote(ref, ref, send_x.at[1, d, e], recv_x.at[1, d, e], peer))
            chain(1, o_mine, o_ref, s, [])
            go(remote(o_ref, o_mine(s), send_y.at[1, s], recv_y.at[1, s], y_peer))
    for k in range(1, sp):
        around(1, o_mine, k, o_beyond)
    for sv in range(sp):
        arrived(recv_t.at[sv], tok_at(sv, 1 - t))
        arrived(recv_y.at[1, sv], o_at(1 - g, sv))
    for d in range(sp):
        sv = lax.rem(s + sp - d, sp)
        for turn, gv in enumerate((g, 1 - g)):
            for e in range(fs - 1):
                fv = lax.rem(f + fs - 1 - e, fs)
                arrived(recv_x.at[turn, d, e], w_at(gv, sv, fv))
    for run, copy in started:
        run(copy.wait_send)
    for copy in keep:
        copy.wait()


def gather_all(normed, w_half, o_half, sp, fs):
    seqs, rows, wide = normed.shape
    any_spec = pl.BlockSpec(memory_space=pl.ANY)
    dma = pltpu.SemaphoreType.DMA
    return pl.pallas_call(
        gather_kernel,
        out_shape=(
            jax.ShapeDtypeStruct((seqs, sp * 2, rows, wide), jnp.bfloat16),
            jax.ShapeDtypeStruct((2, sp * fs) + w_half.shape[1:], jnp.bfloat16),
            jax.ShapeDtypeStruct((2, o_half.shape[0], o_half.shape[1] * sp), jnp.bfloat16),
        ),
        in_specs=[any_spec] * 3,
        out_specs=[any_spec] * 3,
        scratch_shapes=[
            dma((sp,)), dma((sp,)), dma((2, 2, sp)), dma((2, sp)), dma((sp,)), dma((sp,)),
            dma((2, sp, fs - 1)), dma((2, sp, fs - 1)), dma((2, sp)), dma((2, sp)), dma((3,)),
        ],
        compiler_params=pltpu.CompilerParams(collective_id=0, has_side_effects=True),
        name="gather_all",
    )(normed, w_half, o_half)


def merge_kernel(
    attn_ref, conv_ref, o_ref, out_ref, feats, weights, mine, theirs, got, done, landed,
    send, recv, send_x, recv_x, swap, last, local,
):
    sp, fs = lax.axis_size("sp"), lax.axis_size("fs")
    s, t, f = lax.axis_index("sp"), lax.axis_index("tp"), lax.axis_index("fs")
    z_peers = [{"sp": lax.rem(s + d, sp)} for d in range(1, sp)]
    x_peers = [{"fs": lax.rem(f + d, fs)} for d in range(1, fs)]
    t_peer = {"tp": 1 - t}
    greet(z_peers + x_peers + [t_peer])
    seqs, unused, rows, wide = attn_ref.shape
    half = rows // 2
    refs = (attn_ref, conv_ref)
    started = []

    def go(copy):
        copy.start()
        started.append(copy)
        return copy

    for d in range(1, sp):
        to = lax.rem(s + d, sp)
        for kind, ref in enumerate(refs):
            go(
                remote(
                    ref.at[:, to], feats.at[f, kind, s], send.at[kind, d], recv.at[kind, d],
                    {"sp": to},
                )
            )
    for kind, ref in enumerate(refs):
        for e, peer in enumerate(x_peers):
            go(
                remote(
                    ref.at[:, s], feats.at[f, kind, s], send_x.at[kind, 0, e],
                    recv_x.at[kind, 0, e], peer,
                )
            )
    fetch = pltpu.make_async_copy(o_ref, weights, local.at[2])
    fetch.start()
    keep = [
        pltpu.make_async_copy(ref.at[:, s], feats.at[f, kind, s], local.at[kind])
        for kind, ref in enumerate(refs)
    ]
    for copy in keep:
        copy.start()
    for d in range(1, sp):
        sv = lax.rem(s + sp - d, sp)
        for kind in range(2):
            ref = feats.at[f, kind, sv]
            remote(ref, ref, send.at[kind, d], recv.at[kind, d], t_peer).wait_recv()
            for e, peer in enumerate(x_peers):
                go(remote(ref, ref, send_x.at[kind, d, e], recv_x.at[kind, d, e], peer))
    for copy in keep:
        copy.wait()
    fetch.wait()

    def product(fv, tv):
        total = jnp.zeros((seqs * half, weights.shape[2]), jnp.float32)
        for kind in range(2):
            left = jnp.concatenate(
                [
                    feats[fv, kind, sv, :, pl.ds(pl.multiple_of(tv * half, half), half), :].reshape(
                        seqs * half, wide
                    )
                    for sv in range(sp)
                ],
                axis=1,
            )
            total = total + jnp.dot(left, weights[kind], preferred_element_type=jnp.float32)
        return total

    swaps, lasts = [], []
    for e in range(fs):
        fv = lax.rem(f + e, fs)
        if e:
            for d in range(sp):
                sv = lax.rem(s + sp - d, sp)
                for kind in range(2):
                    ref = feats.at[fv, kind, sv]
                    remote(
                        ref, ref, send_x.at[kind, d, fs - 1 - e], recv_x.at[kind, d, fs - 1 - e],
                        t_peer,
                    ).wait_recv()
        theirs[e] = product(fv, 1 - t).astype(jnp.bfloat16)
        swaps.append(
            go(remote(theirs.at[e], got.at[e], swap.at[0, e], swap.at[1, e], t_peer))
        )
        mine[e] = product(fv, t)
    for e in list(range(1, fs)) + [0]:
        swaps[e].wait_recv()
        total = (mine[e] + got[e].astype(jnp.float32)).astype(jnp.bfloat16)
        if e:
            done[e - 1] = total
            lasts.append(
                go(
                    remote(
                        done.at[e - 1], landed.at[e - 1], last.at[0, e - 1], last.at[1, e - 1],
                        x_peers[e - 1],
                    )
                )
            )
        else:
            out_ref[f] = total
    for e in range(1, fs):
        lasts[e - 1].wait_recv()
        out_ref[lax.rem(f + fs - e, fs)] = landed[e - 1]
    for copy in started:
        copy.wait_send()


def merge(attn, conv_out, o_all, fs):
    seqs, sp, rows, wide = attn.shape
    columns = o_all.shape[2]
    lines = seqs * (rows // 2)
    any_spec = pl.BlockSpec(memory_space=pl.ANY)
    dma = pltpu.SemaphoreType.DMA
    out = pl.pallas_call(
        merge_kernel,
        out_shape=jax.ShapeDtypeStruct((fs, lines, columns), jnp.bfloat16),
        in_specs=[any_spec] * 3,
        out_specs=pl.BlockSpec(memory_space=pltpu.VMEM),
        scratch_shapes=[
            pltpu.VMEM((fs, 2, sp, seqs, rows, wide), jnp.bfloat16),
            pltpu.VMEM(o_all.shape, jnp.bfloat16),
            pltpu.VMEM((fs, lines, columns), jnp.float32),
            pltpu.VMEM((fs, lines, columns), jnp.bfloat16),
            pltpu.VMEM((fs, lines, columns), jnp.bfloat16),
            pltpu.VMEM((fs - 1, lines, columns), jnp.bfloat16),
            pltpu.VMEM((fs - 1, lines, columns), jnp.bfloat16),
            dma((2, sp)), dma((2, sp)), dma((2, sp, fs - 1)), dma((2, sp, fs - 1)),
            dma((2, fs)), dma((2, fs - 1)), dma((3,)),
        ],
        compiler_params=pltpu.CompilerParams(collective_id=1, has_side_effects=True),
        name="merge",
    )(attn, conv_out, o_all)
    out = out.reshape(fs, lines, sp, columns // sp).transpose(1, 2, 0, 3)
    return out.reshape(seqs, rows // 2, fs * columns)


def head_map(query, key, value, mix, head_gain):
    seqs, count = value.shape[0], value.shape[1]
    score = jnp.einsum("bqmd,bkmd->bmqk", query, key, preferred_element_type=jnp.float32)
    score = score * DK ** (-0.5)
    place = jnp.arange(count, dtype=jnp.int32)
    score = jnp.where(place[None, :] <= place[:, None], score, NEG)
    weights = jnp.exp(score - jnp.max(score, axis=-1, keepdims=True))
    total = jnp.sum(weights, axis=-1)
    summed = jnp.einsum(
        "bmqk,bkd->bmqd", weights.astype(jnp.bfloat16), value, preferred_element_type=jnp.float32
    )
    mapped = summed / total[..., None]
    return (rms_scale(mapped[:, 0] - mix * mapped[:, 1], head_gain) * OUT_SCALE).astype(jnp.bfloat16)


def heads_on_device(
    tokens, norm_gain, w_query, w_key, w_value, query_gain, key_gain, mix_lambda, head_gain,
    w_gate_b, w_gate_c, w_conv_in, conv_taps, w_out_attn, w_out_conv,
):
    sp, fs = lax.axis_size("sp"), lax.axis_size("fs")
    s, first = lax.axis_index("sp"), lax.axis_index("grp") == 0
    seqs, rows, wide = tokens.shape
    normed = rms_scale(tokens, norm_gain).astype(jnp.bfloat16)
    depth, columns = w_query.shape
    each = columns // sp

    def half(pair):
        return jnp.where(first, pair[0], pair[1])

    picked = [
        half(pair).reshape(depth, sp, each)
        for pair in ((w_query, w_gate_b), (w_key, w_gate_c), (w_value, w_conv_in))
    ]
    w_half = jnp.stack(picked, axis=2).transpose(1, 0, 2, 3).reshape(sp, depth, 3 * each)
    o_half = half((w_out_attn, w_out_conv))
    tok_all, w_all, o_all = gather_all(normed, w_half, o_half, sp, fs)
    count = rows * sp * 2
    x = tok_all.reshape(seqs * count, wide)

    def project(index):
        out = jnp.dot(
            x, w_all[index].reshape(wide, 3 * each), preferred_element_type=jnp.float32
        ).astype(jnp.bfloat16)
        return [out[:, n * each : (n + 1) * each].reshape(seqs, count, each) for n in range(3)]

    query_raw, key_raw, value = project(0)
    gate_b, gate_c, conv_in = project(1)

    def mine(array, axis=0):
        return lax.dynamic_slice_in_dim(array, s * each, each, axis)

    query = rms_scale(
        query_raw.reshape(seqs, count, 2, DK), mine(query_gain).reshape(2, DK)
    ).astype(jnp.bfloat16)
    key = rms_scale(
        key_raw.reshape(seqs, count, 2, DK), mine(key_gain).reshape(2, DK)
    ).astype(jnp.bfloat16)
    mix = lax.dynamic_slice_in_dim(mix_lambda, s, 1)[0]
    attn = head_map(query, key, value, mix, head_gain)
    shaped = (gate_c.astype(jnp.float32) * conv_in.astype(jnp.float32)).astype(jnp.bfloat16)
    padded = jnp.pad(shaped, ((0, 0), (KW - 1, 0), (0, 0))).astype(jnp.float32)
    taps = mine(conv_taps, 1)
    conv = taps[0] * padded[:, 0:count]
    for tap in range(1, KW):
        conv = conv + taps[tap] * padded[:, tap : tap + count]
    conv_out = (gate_b.astype(jnp.float32) * conv).astype(jnp.bfloat16)
    shape = (seqs, sp, rows * 2, each)
    return merge(attn.reshape(shape), conv_out.reshape(shape), o_all, fs)


def on_device(*arrays):
    heads_here, channels = arrays[7].shape[0], arrays[12].shape[1]
    sizes = [lax.axis_size(axis) for axis in ("grp", "tp", "fs", "sp")]
    whole_heads = heads_here == sizes[3] and channels == heads_here * DV
    if whole_heads and sizes[0] == 2 and sizes[1] == 2 and sizes[2] > 1:
        return heads_on_device(*arrays)
    return gather_on_device(*arrays)


def solution(mesh):
    placed = (
        P(("grp", "fs"), ("sp", "tp"), None),
        P(),
        P(("sp", "fs"), "tp"),
        P(("sp", "fs"), "tp"),
        P(("sp", "fs"), "tp"),
        P("tp"),
        P("tp"),
        P("tp"),
        P(),
        P(("sp", "fs"), "tp"),
        P(("sp", "fs"), "tp"),
        P(("sp", "fs"), "tp"),
        P(None, "tp"),
        P("tp", ("sp", "fs")),
        P("tp", ("sp", "fs")),
    )
    return jax.shard_map(
        on_device,
        mesh=mesh,
        in_specs=placed,
        out_specs=P(("grp", "fs"), ("sp", "tp"), None),
        check_vma=False,
    )
```

```python
import functools
import math

import jax
import jax.numpy as jnp
from jax import lax
from jax.experimental import pallas as pl
from jax.experimental.pallas import tpu as pltpu
from jax.sharding import PartitionSpec as P

DK = 64
DV = 128
KW = 3


EPS = 1e-06
NEG = -1e30
OUT_SCALE = 0.8


def from_behind(block, axis, distance):
    devices = range(lax.axis_size(axis))
    route = [(i - distance, i) for i in devices if i - distance in devices]
    return lax.ppermute(block, axis, route)


def rms_scale(values, gain):
    wide = values.astype(jnp.float32)
    return wide * lax.rsqrt(jnp.mean(wide * wide, axis=-1, keepdims=True) + EPS) * gain


def attend_heads(normed, wq_full, wk_full, wv_full, query_gain, key_gain, mix_lambda, head_gain):
    rows = normed.shape[0]
    heads_here = mix_lambda.shape[0]
    query = rms_scale(
        jnp.dot(normed, wq_full, preferred_element_type=jnp.float32)
        .astype(jnp.bfloat16)
        .reshape(rows, heads_here, 2, DK),
        query_gain.reshape(heads_here, 2, DK),
    ).astype(jnp.bfloat16)
    key = rms_scale(
        jnp.dot(normed, wk_full, preferred_element_type=jnp.float32)
        .astype(jnp.bfloat16)
        .reshape(rows, heads_here, 2, DK),
        key_gain.reshape(heads_here, 2, DK),
    ).astype(jnp.bfloat16)
    value = jnp.dot(normed, wv_full, preferred_element_type=jnp.float32).astype(jnp.bfloat16)
    q_pos = lax.axis_index("sp") * rows + jnp.arange(rows, dtype=jnp.int32)
    init = (
        jnp.full((heads_here, 2, rows), NEG, jnp.float32),
        jnp.zeros((heads_here, 2, rows), jnp.float32),
        jnp.zeros((heads_here, 2, rows, DV), jnp.float32),
    )
    key_piece = lax.all_gather(key.reshape(rows, heads_here * 2 * DK), "sp", axis=0, tiled=True)
    value_piece = lax.all_gather(value, "sp", axis=0, tiled=True)
    count = key_piece.shape[0]
    width = math.gcd(count, 1024)
    blocks = count // width
    key_blocks = key_piece.reshape(blocks, width, heads_here, 2, DK)
    value_blocks = value_piece.reshape(blocks, width, heads_here, DV)
    begins = jnp.arange(blocks, dtype=jnp.int32) * width

    def step(state, inputs):
        running, total, summed = state
        key_block, value_block, begin = inputs
        k_pos = begin + jnp.arange(width, dtype=jnp.int32)
        score = jnp.einsum(
            "qhmd,khmd->hmqk", query, key_block, preferred_element_type=jnp.float32
        ) * DK ** (-0.5)
        allowed = k_pos[None, :] <= q_pos[:, None]
        score = jnp.where(allowed, score, NEG)
        newest = jnp.maximum(running, jnp.max(score, axis=-1))
        factor = jnp.exp(running - newest)
        weights = jnp.where(allowed, jnp.exp(score - newest[..., None]), 0.0)
        total = total * factor + jnp.sum(weights, axis=-1)
        summed = summed * factor[..., None] + jnp.einsum(
            "hmqk,khd->hmqd",
            weights.astype(jnp.bfloat16),
            value_block,
            preferred_element_type=jnp.float32,
        )
        return ((newest, total, summed), None)

    result, unused = lax.scan(step, init, (key_blocks, value_blocks, begins))
    running, total, summed = result
    head_map = summed / total[..., None]
    differ = head_map[:, 0] - mix_lambda[:, None, None] * head_map[:, 1]
    normal = rms_scale(differ, head_gain) * OUT_SCALE
    return normal.transpose(1, 0, 2).reshape(rows, heads_here * DV).astype(jnp.bfloat16)


def gated_conv(normed, wb_full, wc_full, wi_full, conv_taps):
    rows = normed.shape[0]
    gate_b = jnp.dot(normed, wb_full, preferred_element_type=jnp.float32).astype(jnp.bfloat16)
    gate_c = jnp.dot(normed, wc_full, preferred_element_type=jnp.float32).astype(jnp.bfloat16)
    conv_in = jnp.dot(normed, wi_full, preferred_element_type=jnp.float32).astype(jnp.bfloat16)
    shaped = (gate_c.astype(jnp.float32) * conv_in.astype(jnp.float32)).astype(jnp.bfloat16)
    edge = from_behind(shaped[rows - (KW - 1) :], "sp", 1)
    padded = jnp.concatenate([edge, shaped], axis=0).astype(jnp.float32)
    conv = conv_taps[0][None, :] * padded[0:rows]
    for tap in range(1, KW):
        conv = conv + conv_taps[tap][None, :] * padded[tap : tap + rows]
    return (gate_b.astype(jnp.float32) * conv).astype(jnp.bfloat16)


def normalize_rows(own_rows, norm_gain):
    return rms_scale(lax.all_gather(own_rows, "tp", axis=0, tiled=True), norm_gain).astype(
        jnp.bfloat16
    )


def gather_on_device(
    tokens,
    norm_gain,
    w_query,
    w_key,
    w_value,
    query_gain,
    key_gain,
    mix_lambda,
    head_gain,
    w_gate_b,
    w_gate_c,
    w_conv_in,
    conv_taps,
    w_out_attn,
    w_out_conv,
):
    seq_count = tokens.shape[0]
    gathered = (
        lax.all_gather(w_query, ("sp", "fs"), axis=0, tiled=True),
        lax.all_gather(w_key, ("sp", "fs"), axis=0, tiled=True),
        lax.all_gather(w_value, ("sp", "fs"), axis=0, tiled=True),
        lax.all_gather(w_gate_b, ("sp", "fs"), axis=0, tiled=True),
        lax.all_gather(w_gate_c, ("sp", "fs"), axis=0, tiled=True),
        lax.all_gather(w_conv_in, ("sp", "fs"), axis=0, tiled=True),
        lax.all_gather(w_out_attn, ("sp", "fs"), axis=1, tiled=True),
        lax.all_gather(w_out_conv, ("sp", "fs"), axis=1, tiled=True),
    )
    normed_list = [normalize_rows(tokens[index], norm_gain) for index in range(seq_count)]
    attn_list = [
        attend_heads(
            normed,
            gathered[0],
            gathered[1],
            gathered[2],
            query_gain,
            key_gain,
            mix_lambda,
            head_gain,
        )
        for normed in normed_list
    ]
    conv_list = [
        gated_conv(normed, gathered[3], gathered[4], gathered[5], conv_taps)
        for normed in normed_list
    ]
    out_attn = gathered[6]
    out_conv = gathered[7]
    results = []
    for index in range(seq_count):
        attn = attn_list[index]
        conv_out = conv_list[index]
        results.append(
            lax.psum_scatter(
                (
                    jnp.dot(attn, out_attn, preferred_element_type=jnp.float32)
                    + jnp.dot(conv_out, out_conv, preferred_element_type=jnp.float32)
                ).astype(jnp.bfloat16),
                "tp",
                scatter_dimension=0,
                tiled=True,
            )
        )
    return jnp.stack(results, axis=0)


MESH = pl.DeviceIdType.MESH


def greet(peers):
    barrier = pltpu.get_barrier_semaphore()
    for peer in peers:
        pl.semaphore_signal(barrier, inc=1, device_id=peer, device_id_type=MESH)
    pl.semaphore_wait(barrier, len(peers))


def remote(src, dst, send, recv, peer):
    return pltpu.make_async_remote_copy(
        src_ref=src, dst_ref=dst, send_sem=send, recv_sem=recv, device_id=peer, device_id_type=MESH
    )


def layer_kernel(
    tok_ref, w_ref, o_ref, small_ref, out_ref, tok_all, w_all, o_all, padded, own, feats,
    mine, theirs, got, done, landed,
    send_z, recv_z, send_c, recv_c, send_t, recv_t, send_x, recv_x, send_y, recv_y, local,
    send_f, recv_f, send_g, recv_g, swap, last,
):
    sp, fs = lax.axis_size("sp"), lax.axis_size("fs")
    s, f = lax.axis_index("sp"), lax.axis_index("fs")
    g, t = lax.axis_index("grp"), lax.axis_index("tp")
    width = o_ref.shape[1]
    z_peers = [{"sp": lax.rem(s + d, sp)} for d in range(1, sp)]
    x_peers = [{"fs": lax.rem(f + d, fs)} for d in range(1, fs)]
    y_peer = {"grp": 1 - g}
    t_peer = {"tp": 1 - t}
    greet(z_peers + x_peers + [y_peer, t_peer])

    def tok_at(sv, tv):
        return tok_all.at[:, sv * 2 + tv]

    def w_at(gv, sv, fv):
        return w_all.at[gv, sv * fs + fv]

    def o_at(gv, sv):
        return o_all.at[gv, :, pl.ds(pl.multiple_of(sv * width, 128), width)]

    started = []

    def go(copy, needs=()):
        def run(act):
            if needs:
                pl.when(functools.reduce(jnp.logical_and, needs))(act)
            else:
                act()

        run(copy.start)
        started.append((run, copy))

    def arrived(sem, ref, needs=()):
        copy = remote(ref, ref, sem, sem, t_peer)
        if needs:
            pl.when(functools.reduce(jnp.logical_and, needs))(copy.wait_recv)
        else:
            copy.wait_recv()

    def chain(kind, at, src, sv, needs):
        ref = at(sv)
        for way, (to, moves) in enumerate(((s + 1, sv <= s), (s - 1, sv >= s))):
            fits = to < sp if way == 0 else to >= 0
            peer = {"sp": jnp.clip(to, 0, sp - 1)}
            go(
                remote(src, ref, send_c.at[kind, way, sv], recv_c.at[kind, sv], peer),
                needs + [fits, moves],
            )

    def spread_w(d, src):
        sv = lax.rem(s + sp - d, sp)
        for e, peer in enumerate(x_peers):
            go(remote(src, w_at(g, sv, f), send_x.at[0, d, e], recv_x.at[0, d, e], peer))
        go(remote(src, w_at(g, sv, f), send_y.at[0, d], recv_y.at[0, d], y_peer))

    def tok_mine(sv):
        return tok_at(sv, t)

    def o_mine(sv):
        return o_at(g, sv)

    for d in range(1, sp):
        to = lax.rem(s + d, sp)
        go(remote(w_ref.at[to], w_at(g, s, f), send_z.at[d], recv_z.at[d], {"sp": to}))
    chain(0, tok_mine, tok_ref, s, [])
    spread_w(0, w_ref.at[s])
    go(remote(tok_ref, tok_mine(s), send_t.at[s], recv_t.at[s], t_peer))
    keep = [
        pltpu.make_async_copy(tok_ref, tok_at(s, t), local.at[0]),
        pltpu.make_async_copy(w_ref.at[s], w_at(g, s, f), local.at[1]),
        pltpu.make_async_copy(o_ref, o_at(g, s), local.at[2]),
    ]
    for copy in keep:
        copy.start()
    for d in range(1, sp):
        ref = w_at(g, lax.rem(s + sp - d, sp), f)
        arrived(recv_z.at[d], ref)
        spread_w(d, ref)

    def around(kind, at, distance, beyond):
        for shift in (-distance, distance):
            sv = jnp.clip(s + shift, 0, sp - 1)
            there = (s + shift >= 0) if shift < 0 else (s + shift < sp)
            ref = at(sv)
            arrived(recv_c.at[kind, sv], ref, [there])
            if shift < 0:
                to, fits, way = s + 1, s + 1 < sp, 0
            else:
                to, fits, way = s - 1, s - 1 >= 0, 1
            peer = {"sp": jnp.clip(to, 0, sp - 1)}
            go(
                remote(ref, ref, send_c.at[kind, way, sv], recv_c.at[kind, sv], peer),
                [there, fits],
            )
            beyond(sv, ref, there)

    def tok_beyond(sv, ref, there):
        go(remote(ref, ref, send_t.at[sv], recv_t.at[sv], t_peer), [there])

    def o_beyond(sv, ref, there):
        go(remote(ref, ref, send_y.at[1, sv], recv_y.at[1, sv], y_peer), [there])

    for k in range(1, sp):
        around(0, tok_mine, k, tok_beyond)
        if k == 1:
            for d in range(sp):
                ref = w_at(1 - g, lax.rem(s + sp - d, sp), f)
                arrived(recv_y.at[0, d], ref)
                for e, peer in enumerate(x_peers):
                    go(remote(ref, ref, send_x.at[1, d, e], recv_x.at[1, d, e], peer))
            chain(1, o_mine, o_ref, s, [])
            go(remote(o_ref, o_mine(s), send_y.at[1, s], recv_y.at[1, s], y_peer))
    for sv in range(sp):
        arrived(recv_t.at[sv], tok_at(sv, 1 - t))
    for d in range(sp):
        sv = lax.rem(s + sp - d, sp)
        for turn, gv in enumerate((g, 1 - g)):
            for e in range(fs - 1):
                fv = lax.rem(f + fs - 1 - e, fs)
                arrived(recv_x.at[turn, d, e], w_at(gv, sv, fv))
    for copy in keep:
        copy.wait()
    around(1, o_mine, 1, o_beyond)

    seqs, shards, part, wide = tok_all.shape
    count, each = shards * part, own.shape[4]
    rows = count // sp
    depth = w_all.shape[1] * w_all.shape[2]

    def project(b, index):
        out = jnp.dot(
            tok_all[b].reshape(count, wide),
            w_all[index].reshape(depth, 3 * each),
            preferred_element_type=jnp.float32,
        ).astype(jnp.bfloat16)
        return [out[:, n * each : (n + 1) * each] for n in range(3)]

    def send_feats(b):
        for d in range(1, sp):
            to = lax.rem(s + d, sp)
            go(
                remote(
                    own.at[b, to], feats.at[f, s, b], send_f.at[b, d], recv_f.at[b, d], {"sp": to}
                )
            )
        for e, peer in enumerate(x_peers):
            go(
                remote(
                    own.at[b, s], feats.at[f, s, b], send_g.at[b, 0, e], recv_g.at[b, 0, e], peer
                )
            )

    def relay_feats(b):
        for d in range(1, sp):
            ref = feats.at[f, lax.rem(s + sp - d, sp), b]
            arrived(recv_f.at[b, d], ref)
            for e, peer in enumerate(x_peers):
                go(remote(ref, ref, send_g.at[b, d, e], recv_g.at[b, d, e], peer))

    first = lax.broadcasted_iota(jnp.int32, (count, each), 1) < DK

    def pair_norm(raw, gain):
        value = raw.astype(jnp.float32)
        square = value * value
        low = jnp.sum(jnp.where(first, square, 0.0), axis=-1, keepdims=True) * (1.0 / DK)
        high = jnp.sum(jnp.where(first, 0.0, square), axis=-1, keepdims=True) * (1.0 / DK)
        return value * jnp.where(first, lax.rsqrt(low + EPS), lax.rsqrt(high + EPS)) * gain

    def attend(b):
        query_raw, key_raw, value = project(b, 0)
        query = pair_norm(query_raw, small_ref[0:1])
        key = pair_norm(key_raw, small_ref[1:2]).astype(jnp.bfloat16)
        pairs = [
            jnp.where(first, query, 0.0).astype(jnp.bfloat16),
            jnp.where(first, 0.0, query).astype(jnp.bfloat16),
        ]
        for i in range(sp):
            seen = (i + 1) * rows
            row = lax.broadcasted_iota(jnp.int32, (rows, seen), 0) + i * rows
            allowed = lax.broadcasted_iota(jnp.int32, (rows, seen), 1) <= row
            maps = []
            for pair in pairs:
                score = lax.dot_general(
                    pair[i * rows : seen], key[:seen], (((1,), (1,)), ((), ())),
                    preferred_element_type=jnp.float32,
                ) * DK ** (-0.5)
                score = jnp.where(allowed, score, NEG)
                weights = jnp.exp(score - jnp.max(score, axis=-1, keepdims=True))
                total = jnp.sum(weights, axis=-1, keepdims=True)
                summed = jnp.dot(
                    weights.astype(jnp.bfloat16), value[:seen], preferred_element_type=jnp.float32
                )
                maps.append(summed / total)
            differ = maps[0] - small_ref[3:4] * maps[1]
            scale = lax.rsqrt(jnp.mean(differ * differ, axis=-1, keepdims=True) + EPS)
            own[b, i, 0] = (differ * scale * small_ref[2:3] * OUT_SCALE).astype(jnp.bfloat16)

    def convolve(b):
        gate_b, gate_c, conv_in = project(b, 1)
        shaped = (gate_c.astype(jnp.float32) * conv_in.astype(jnp.float32)).astype(jnp.bfloat16)
        front = padded.shape[0] - count
        padded[0:front] = jnp.zeros((front, each), jnp.float32)
        padded[front:] = shaped.astype(jnp.float32)
        conv = jnp.zeros((count, each), jnp.float32)
        for tap in range(KW):
            begin = front - (KW - 1) + tap
            conv = conv + small_ref[4 + tap : 5 + tap] * padded[begin : begin + count]
        conv_out = (gate_b.astype(jnp.float32) * conv).astype(jnp.bfloat16)
        for i in range(sp):
            own[b, i, 1] = conv_out[i * rows : (i + 1) * rows]

    o_turns = list(range(2, sp))
    for b in range(seqs):
        convolve(b)
        if o_turns:
            around(1, o_mine, o_turns.pop(0), o_beyond)
        attend(b)
        if o_turns:
            around(1, o_mine, o_turns.pop(0), o_beyond)
        send_feats(b)
        if b:
            relay_feats(b - 1)
    for k in o_turns:
        around(1, o_mine, k, o_beyond)
    for b in range(seqs):
        keep = pltpu.make_async_copy(own.at[b, s], feats.at[f, s, b], local.at[3 + b])
        keep.start()
    relay_feats(seqs - 1)
    for b in range(seqs):
        pltpu.make_async_copy(own.at[b, s], feats.at[f, s, b], local.at[3 + b]).wait()
    for sv in range(sp):
        arrived(recv_y.at[1, sv], o_at(1 - g, sv))
    half = rows // 2
    lines = seqs * half

    def product(fv, tv):
        total = jnp.zeros((lines, o_all.shape[2]), jnp.float32)
        for kind in range(2):
            left = jnp.concatenate(
                [
                    feats[
                        fv, sv, :, kind, pl.ds(pl.multiple_of(tv * half, half), half), :
                    ].reshape(lines, each)
                    for sv in range(sp)
                ],
                axis=1,
            )
            total = total + jnp.dot(left, o_all[kind], preferred_element_type=jnp.float32)
        return total

    swaps, lasts = [], []
    for e in range(fs):
        fv = lax.rem(f + e, fs)
        if e:
            for d in range(sp):
                sv = lax.rem(s + sp - d, sp)
                for b in range(seqs):
                    arrived(recv_g.at[b, d, fs - 1 - e], feats.at[fv, sv, b])
        theirs[e] = product(fv, 1 - t).astype(jnp.bfloat16)
        copy = remote(theirs.at[e], got.at[e], swap.at[0, e], swap.at[1, e], t_peer)
        go(copy)
        swaps.append(copy)
        mine[e] = product(fv, t)
    for e in list(range(1, fs)) + [0]:
        swaps[e].wait_recv()
        total = (mine[e] + got[e].astype(jnp.float32)).astype(jnp.bfloat16)
        if e:
            done[e - 1] = total
            copy = remote(
                done.at[e - 1], landed.at[e - 1], last.at[0, e - 1], last.at[1, e - 1],
                x_peers[e - 1],
            )
            go(copy)
            lasts.append(copy)
        else:
            out_ref[f] = total
    for e in range(1, fs):
        lasts[e - 1].wait_recv()
        out_ref[lax.rem(f + fs - e, fs)] = landed[e - 1]
    for run, copy in started:
        run(copy.wait_send)


def layer(normed, w_half, o_half, small, sp, fs):
    seqs, part, wide = normed.shape
    rows, each = part * 2, w_half.shape[2] // 3
    count, lines = rows * sp, seqs * part
    columns = o_half.shape[1] * sp
    any_spec = pl.BlockSpec(memory_space=pl.ANY)
    vmem_spec = pl.BlockSpec(memory_space=pltpu.VMEM)
    dma = pltpu.SemaphoreType.DMA
    narrow = functools.partial(pltpu.VMEM, dtype=jnp.bfloat16)
    out = pl.pallas_call(
        layer_kernel,
        out_shape=jax.ShapeDtypeStruct((fs, lines, columns), jnp.bfloat16),
        in_specs=[any_spec] * 3 + [vmem_spec],
        out_specs=vmem_spec,
        scratch_shapes=[
            narrow((seqs, sp * 2, part, wide)),
            narrow((2, sp * fs) + w_half.shape[1:]),
            narrow((2, o_half.shape[0], columns)),
            pltpu.VMEM((count + 8, each), jnp.float32),
            narrow((seqs, sp, 2, rows, each)),
            narrow((fs, sp, seqs, 2, rows, each)),
            pltpu.VMEM((fs, lines, columns), jnp.float32),
            narrow((fs, lines, columns)),
            narrow((fs, lines, columns)),
            narrow((fs - 1, lines, columns)),
            narrow((fs - 1, lines, columns)),
            dma((sp,)), dma((sp,)), dma((2, 2, sp)), dma((2, sp)), dma((sp,)), dma((sp,)),
            dma((2, sp, fs - 1)), dma((2, sp, fs - 1)), dma((2, sp)), dma((2, sp)),
            dma((3 + seqs,)),
            dma((seqs, sp)), dma((seqs, sp)), dma((seqs, sp, fs - 1)), dma((seqs, sp, fs - 1)),
            dma((2, fs)), dma((2, fs - 1)),
        ],
        compiler_params=pltpu.CompilerParams(collective_id=0, has_side_effects=True),
        name="layer",
    )(normed, w_half, o_half, small)
    out = out.reshape(fs, lines, sp, columns // sp).transpose(1, 2, 0, 3)
    return out.reshape(seqs, part, fs * columns)


def heads_on_device(
    tokens, norm_gain, w_query, w_key, w_value, query_gain, key_gain, mix_lambda, head_gain,
    w_gate_b, w_gate_c, w_conv_in, conv_taps, w_out_attn, w_out_conv,
):
    sp, fs = lax.axis_size("sp"), lax.axis_size("fs")
    s, first = lax.axis_index("sp"), lax.axis_index("grp") == 0
    seqs, rows, wide = tokens.shape
    normed = rms_scale(tokens, norm_gain).astype(jnp.bfloat16)
    depth, columns = w_query.shape
    each = columns // sp

    def half(pair):
        return jnp.where(first, pair[0], pair[1])

    picked = [
        half(pair).reshape(depth, sp, each)
        for pair in ((w_query, w_gate_b), (w_key, w_gate_c), (w_value, w_conv_in))
    ]
    w_half = jnp.stack(picked, axis=2).transpose(1, 0, 2, 3).reshape(sp, depth, 3 * each)
    o_half = half((w_out_attn, w_out_conv))

    def mine(array, axis=0):
        return lax.dynamic_slice_in_dim(array, s * each, each, axis)

    mix = lax.dynamic_slice_in_dim(mix_lambda, s, 1)
    small = jnp.concatenate(
        [
            mine(query_gain)[None],
            mine(key_gain)[None],
            head_gain[None],
            jnp.broadcast_to(mix[:, None], (1, each)),
            mine(conv_taps, 1),
        ]
    )
    return layer(normed, w_half, o_half, small, sp, fs)


def on_device(*arrays):
    heads_here, channels = arrays[7].shape[0], arrays[12].shape[1]
    sizes = [lax.axis_size(axis) for axis in ("grp", "tp", "fs", "sp")]
    whole_heads = heads_here == sizes[3] and channels == heads_here * DV
    if whole_heads and sizes[0] == 2 and sizes[1] == 2 and sizes[2] > 1:
        return heads_on_device(*arrays)
    return gather_on_device(*arrays)


def solution(mesh):
    placed = (
        P(("grp", "fs"), ("sp", "tp"), None),
        P(),
        P(("sp", "fs"), "tp"),
        P(("sp", "fs"), "tp"),
        P(("sp", "fs"), "tp"),
        P("tp"),
        P("tp"),
        P("tp"),
        P(),
        P(("sp", "fs"), "tp"),
        P(("sp", "fs"), "tp"),
        P(("sp", "fs"), "tp"),
        P(None, "tp"),
        P("tp", ("sp", "fs")),
        P("tp", ("sp", "fs")),
    )
    return jax.shard_map(
        on_device,
        mesh=mesh,
        in_specs=placed,
        out_specs=P(("grp", "fs"), ("sp", "tp"), None),
        check_vma=False,
    )
```
